32 devices in a mesh: grp: 2 (over x), ep: 16 (over z, y, core).
Axes of the slice: x: 2, y: 2, z: 4, core: 2. Of those that a mesh axis runs over, the one named last changes fastest.
Arguments:
- tokens: bfloat16 [128, 2048], P(('grp', 'ep')), parts along dimension 0, may hold values from -6 to 6
- prior_state: float32 [128, 32, 64, 64], P(('grp', 'ep')), parts along dimension 0, may hold values from -3 to 3
- receptance_matrix: bfloat16 [2048, 2048], P('ep'), may hold values from -0.125 to 0.125
- key_matrix: bfloat16 [2048, 2048], P('ep'), may hold values from -0.125 to 0.125
- value_matrix: bfloat16 [2048, 2048], P('ep'), may hold values from -0.125 to 0.125
- decay_lowrank_first: bfloat16 [2048, 64], replicated, may hold values from -0.125 to 0.125
- decay_lowrank_second: bfloat16 [64, 2048], replicated, may hold values from -1.5 to 1.5
- decay_channel_offset: float32 [2048], replicated, may hold values from -6 to 0
- correction_lowrank_first: bfloat16 [2048, 64], replicated, may hold values from -0.125 to 0.125
- correction_lowrank_second: bfloat16 [64, 2048], replicated, may hold values from -1.5 to 1.5
- correction_offset: float32 [2048], replicated, may hold values from -4 to 4
- gate_lowrank_first: bfloat16 [2048, 128], replicated, may hold values from -0.25 to 0.25
- gate_lowrank_second: bfloat16 [128, 2048], replicated, may hold values from -0.5 to 0.5
- key_rate_blend: float32 [2048], replicated, may hold values from 0.1 to 1.9
- self_token_scale: float32 [32, 64], replicated, may hold values from -1.2 to 1.2
- per_head_gain: float32 [2048], replicated, may hold values from 0.1 to 1.9
- per_head_bias: float32 [2048], replicated, may hold values from -1.8 to 1.8
- mixer_output_weight: bfloat16 [2048, 2048], P('ep'), may hold values from -0.125 to 0.125
- mixer_norm_gain: float32 [2048], replicated, may hold values from 0.1 to 1.9
- mixer_norm_bias: float32 [2048], replicated, may hold values from -1.8 to 1.8
- expert_norm_gain: float32 [2048], replicated, may hold values from 0.1 to 1.9
- expert_norm_bias: float32 [2048], replicated, may hold values from -1.8 to 1.8
- routes: int32 [128, 4], P(('grp', 'ep')), parts along dimension 0, may hold values from 0 to 15, all different within a row; in each aligned block of 4 rows (0 to 3, 4 to 7, ...) at most 2 rows name the same one
- routing_weight: float32 [128, 4], P(('grp', 'ep')), parts along dimension 0, may hold values from 0.1 to 1
- expert_gate_weight: bfloat16 [16, 2048, 512], P('ep'), may hold values from -0.125 to 0.125
- expert_up_weight: bfloat16 [16, 2048, 512], P('ep'), may hold values from -0.125 to 0.125
- expert_down_weight: bfloat16 [16, 512, 2048], P('ep'), may hold values from -0.25 to 0.25
Outputs:
- result: bfloat16 [128, 2048], P(('grp', 'ep')), parts along dimension 0
- next_state: float32 [128, 32, 64, 64], P(('grp', 'ep')), parts along dimension 0
The draws below stay inside these ranges and needn't reach their ends.
There are 2 independent parts, one for each index of `grp`. The reference program is written for one: setup_inputs(seed, part) draws one part's arguments, and reference() takes and returns one part's arrays. A program takes and returns all parts, laid end to end along the dimension named above; an argument that names none is the same for every part. Nothing has to cross between parts.
Inputs may be any that keep to these rules, and one draw needn't show every extreme that they name: `routes`: A row names 4 different experts. Among the rows of one device no expert is named more than 2 times, and in some device one expert is named exactly 2 times; every expert is named somewhere.
All inputs are finite; a program needn't handle non-finite values.
Results may differ from the reference program's by a relative error of at most 0.0081.
Values may be sent and summed in bfloat16 or wider, within the bound.
A program may use at most 128 MiB of HBM per device.

```python
import math
import jax
import jax.numpy as jnp
import numpy as np
from jax import lax

D = 2048
MIXER_HEADS = 32
HEAD_CHANNELS = 64
W = 2048
DECAY_RANK = 64
LEARN_RANK = 64
GATE_RANK = 128
FF = 512
TOP = 4
SEQ_DEV = 4
TOKENS = 64
EXPERTS = 16
CAP = 2
N_EP = 16


def levels(own_key, extent, cuts, smallest, largest):
    factor_of, own = 1.0, jax.random.fold_in(own_key, 6)
    for axis_at, shards_of in cuts:
        heights = jnp.exp(jax.random.uniform(jax.random.fold_in(own, axis_at), (shards_of,), jnp.float32, smallest / len(cuts), largest / len(cuts)))
        factor_of = factor_of * jnp.repeat(heights, extent[axis_at] // shards_of).reshape([-1 if axis == axis_at else 1 for axis in range(len(extent))])
    return factor_of


def assign_block(rng, own, number, rows, number_of, top, reach, slope):
    order = jax.random.permutation(rng, number_of)
    heavy_load, usual = shares(number_of, rows * top, reach, slope, True), shares(number_of, rows * top, reach, slope, False)
    places = jnp.arange(number_of)

    def named(lengths, turn):
        used = int((lengths > 0).sum())
        fixed = max(1, used // 4)
        moved = fixed + (places - fixed + turn * (used - fixed)) % max(1, number_of - fixed)
        return jnp.zeros((number_of,), jnp.int32).at[order[jnp.where(places < fixed, places, moved)]].set(jnp.asarray(lengths, jnp.int32))

    lengths = jnp.where(number % 4 == 0, named(heavy_load, number // 4), named(usual, number - number // 4 - 1))
    mixed = jax.random.permutation(jax.random.fold_in(own, 3), number_of)
    source_of, receiver = mixed[0:number_of // 2 * 2:2], mixed[1:number_of // 2 * 2:2]
    room = jnp.minimum(lengths[source_of] - 1, reach - lengths[receiver]) // 2
    room = jnp.where((source_of == order[0]) | (receiver == order[0]) | (lengths[receiver] == 0), 0, jnp.maximum(room, 0))
    moved = jax.random.randint(jax.random.fold_in(own, 4), (number_of // 2,), 0, 1 << 20) % (room + 1)
    lengths = lengths.at[source_of].add(-moved).at[receiver].add(moved)
    labels = jnp.searchsorted(jnp.cumsum(lengths), jnp.arange(rows * top), side="right").astype(jnp.int32)
    listing = labels.reshape(top, rows).T
    listing = listing[jax.random.permutation(jax.random.fold_in(own, 1), rows)]
    turn = jax.random.randint(jax.random.fold_in(own, 2), (rows, 1), 0, top)
    return jnp.take_along_axis(listing, (jnp.arange(top)[None, :] + turn) % top, axis=1)


def shares(number_of, total, reach, lean, full):
    weights = [(1 << 20) // math.isqrt(standing ** lean) + 1 for standing in range(1, number_of + 1)]
    largest = reach if full else min(reach, max(-(-total // number_of), total * weights[0] // sum(weights)))
    least = 1 if total - largest >= number_of - 1 else 0
    given, spare = [largest] + [least] * (number_of - 1), total - largest - least * (number_of - 1)
    while spare > 0:
        free = [i for i in range(1, number_of) if given[i] < largest] or [i for i in range(1, number_of) if given[i] < reach]
        mass, remaining = sum([weights[i] for i in free]), spare
        for i in free:
            extra = min(reach - given[i], max(1, remaining * weights[i] // mass), spare)
            given[i] = given[i] + extra
            spare = spare - extra
    return np.array(given)


def noise(stream_key, extent, scale, limit, split=(), kind=jnp.bfloat16):
    factor_of = levels(stream_key, extent, split, -0.22, 0.18) if split else 1.0
    values = jax.random.normal(stream_key, extent, jnp.float32) * scale * factor_of
    return jnp.minimum(jnp.maximum(values, -limit), limit).astype(kind)


def setup_inputs(seed: int = 0, part: int = 0) -> dict:
    arg_keys = jax.random.split(jax.random.key(seed), 28)
    part_keys = jax.random.split(jax.random.fold_in(arg_keys[27], part), 28)
    tokens = noise(part_keys[0], (TOKENS, D), 1.0, 6.0, ((0, 16),))
    prior_state = noise(part_keys[1], (TOKENS, MIXER_HEADS, HEAD_CHANNELS, HEAD_CHANNELS), 0.3, 3.0, ((0, 16),), jnp.float32)
    receptance_matrix = noise(arg_keys[2], (D, W), D ** -0.5, 0.125, ((0, 16),))
    key_matrix = noise(arg_keys[3], (D, W), D ** -0.5, 0.125, ((0, 16),))
    value_matrix = noise(arg_keys[4], (D, W), D ** -0.5, 0.125, ((0, 16),))
    decay_lowrank_first = noise(arg_keys[5], (D, DECAY_RANK), D ** -0.5, 0.125)
    decay_lowrank_second = noise(arg_keys[6], (DECAY_RANK, W), (DECAY_RANK // 4) ** -0.5, 1.5)
    decay_channel_offset = jnp.clip(jax.random.uniform(arg_keys[7], (W,), jnp.float32, -6.0, 0.0), -6.0, 0.0)
    correction_lowrank_first = noise(arg_keys[8], (D, LEARN_RANK), D ** -0.5, 0.125)
    correction_lowrank_second = noise(arg_keys[9], (LEARN_RANK, W), (LEARN_RANK // 4) ** -0.5, 1.5)
    correction_offset = noise(arg_keys[10], (W,), 1.0, 4.0, (), jnp.float32)
    gate_lowrank_first = noise(arg_keys[11], (D, GATE_RANK), (D // 4) ** -0.5, 0.25)
    gate_lowrank_second = noise(arg_keys[12], (GATE_RANK, W), GATE_RANK ** -0.5, 0.5)
    key_rate_blend = jnp.clip(1.0 + 0.18 * jax.random.normal(arg_keys[13], (W,), jnp.float32), 0.1, 1.9)
    self_token_scale = noise(arg_keys[14], (MIXER_HEADS, HEAD_CHANNELS), 0.2, 1.2, (), jnp.float32)
    per_head_gain = jnp.clip(1.0 + 0.18 * jax.random.normal(arg_keys[15], (W,), jnp.float32), 0.1, 1.9)
    per_head_bias = noise(arg_keys[16], (W,), 0.3, 1.8, (), jnp.float32)
    mixer_output_weight = noise(arg_keys[17], (W, D), W ** -0.5, 0.125, ((0, 16),))
    mixer_norm_gain = jnp.clip(1.0 + 0.18 * jax.random.normal(arg_keys[18], (D,), jnp.float32), 0.1, 1.9)
    mixer_norm_bias = noise(arg_keys[19], (D,), 0.3, 1.8, (), jnp.float32)
    expert_norm_gain = jnp.clip(1.0 + 0.18 * jax.random.normal(arg_keys[20], (D,), jnp.float32), 0.1, 1.9)
    expert_norm_bias = noise(arg_keys[21], (D,), 0.3, 1.8, (), jnp.float32)
    routes_keys = jax.random.split(jax.random.fold_in(part_keys[22], 1), TOKENS // SEQ_DEV)
    routes_turns = jax.random.permutation(jax.random.fold_in(part_keys[22], 3), TOKENS // SEQ_DEV)
    routes = jax.vmap(lambda own, number: assign_block(jax.random.fold_in(part_keys[22], 2), own, number, SEQ_DEV, EXPERTS, TOP, CAP, 1))(routes_keys, routes_turns).reshape((TOKENS, TOP))
    routing_weight = jnp.clip(0.1 + 0.9 * jax.random.uniform(part_keys[23], (TOKENS, TOP), jnp.float32) ** levels(part_keys[23], (TOKENS, TOP), ((0, 16),), -0.2, 0.2), 0.1, 1.0)
    expert_gate_weight = noise(arg_keys[24], (EXPERTS, D, FF), D ** -0.5, 0.125, ((0, 16),))
    expert_up_weight = noise(arg_keys[25], (EXPERTS, D, FF), D ** -0.5, 0.125, ((0, 16),))
    expert_down_weight = noise(arg_keys[26], (EXPERTS, FF, D), FF ** -0.5, 0.25, ((0, 16),))
    return {"tokens": tokens, "prior_state": prior_state, "receptance_matrix": receptance_matrix, "key_matrix": key_matrix, "value_matrix": value_matrix, "decay_lowrank_first": decay_lowrank_first, "decay_lowrank_second": decay_lowrank_second, "decay_channel_offset": decay_channel_offset, "correction_lowrank_first": correction_lowrank_first, "correction_lowrank_second": correction_lowrank_second, "correction_offset": correction_offset, "gate_lowrank_first": gate_lowrank_first, "gate_lowrank_second": gate_lowrank_second, "key_rate_blend": key_rate_blend, "self_token_scale": self_token_scale, "per_head_gain": per_head_gain, "per_head_bias": per_head_bias, "mixer_output_weight": mixer_output_weight, "mixer_norm_gain": mixer_norm_gain, "mixer_norm_bias": mixer_norm_bias, "expert_norm_gain": expert_norm_gain, "expert_norm_bias": expert_norm_bias, "routes": routes, "routing_weight": routing_weight, "expert_gate_weight": expert_gate_weight, "expert_up_weight": expert_up_weight, "expert_down_weight": expert_down_weight}


def layer_norm(values_in, gain_vec, bias_vec):
    row_mean = lax.optimization_barrier(jnp.mean(values_in, -1, keepdims=True))
    centered = values_in - row_mean
    row_var = lax.optimization_barrier(jnp.mean(centered * centered, -1, keepdims=True))
    return centered * lax.rsqrt(row_var + 1e-05) * gain_vec + bias_vec

def recurrent_readout(tokens, prior_state, receptance_rows, key_rows, value_rows, decay_lowrank_first, decay_lowrank_second, decay_channel_offset, correction_lowrank_first, correction_lowrank_second, correction_offset, gate_lowrank_first, gate_lowrank_second, key_rate_blend, self_token_scale, per_head_gain, per_head_bias):
    row_count = tokens.shape[0]
    head_count = prior_state.shape[1]
    head_size = prior_state.shape[2]
    squash = jnp.tanh(jnp.dot(tokens, decay_lowrank_first, preferred_element_type=jnp.float32)).astype(jnp.bfloat16)
    pre_decay = decay_channel_offset + jnp.dot(squash, decay_lowrank_second, preferred_element_type=jnp.float32)
    decay_rate = jnp.exp(-jnp.exp(-jax.nn.softplus(-pre_decay) - 0.5))
    low_learn = jnp.dot(tokens, correction_lowrank_first, preferred_element_type=jnp.float32).astype(jnp.bfloat16)
    learn_rate = jax.nn.sigmoid(correction_offset + jnp.dot(low_learn, correction_lowrank_second, preferred_element_type=jnp.float32))
    opened = jax.nn.sigmoid(jnp.dot(tokens, gate_lowrank_first, preferred_element_type=jnp.float32)).astype(jnp.bfloat16)
    gating = jnp.dot(opened, gate_lowrank_second, preferred_element_type=jnp.float32)

    def by_head(flat_arr):
        return flat_arr.reshape(row_count, head_count, head_size)
    scaled = by_head(key_rows)
    unit_key = scaled * lax.rsqrt(lax.optimization_barrier(jnp.sum(scaled * scaled, -1, keepdims=True)) + 1e-06)
    written_key = by_head(key_rows * (1.0 + (learn_rate - 1.0) * key_rate_blend))
    receptance_by_head = by_head(receptance_rows)
    value_by_head = by_head(value_rows)
    removed = jnp.einsum('nhvk,nhk->nhv', prior_state, unit_key, precision=lax.Precision.HIGHEST)
    next_state = prior_state * by_head(decay_rate)[:, :, None, :] - removed[..., None] * (unit_key * by_head(learn_rate))[:, :, None, :] + value_by_head[..., None] * written_key[:, :, None, :]
    readout = jnp.einsum('nhvk,nhk->nhv', next_state, receptance_by_head, precision=lax.Precision.HIGHEST)
    head_mean = lax.optimization_barrier(jnp.mean(readout, -1, keepdims=True))
    head_dev = readout - head_mean
    head_var = lax.optimization_barrier(jnp.mean(head_dev * head_dev, -1, keepdims=True))
    normed = (head_dev * lax.rsqrt(head_var + 0.00064)).reshape(row_count, -1) * per_head_gain + per_head_bias
    self_token_term = lax.optimization_barrier(jnp.sum(receptance_by_head * written_key * self_token_scale, -1, keepdims=True)) * value_by_head
    mixer_result = ((normed + self_token_term.reshape(row_count, -1)) * gating).astype(jnp.bfloat16)
    return (mixer_result, next_state)

def reference(tokens, prior_state, receptance_matrix, key_matrix, value_matrix, decay_lowrank_first, decay_lowrank_second, decay_channel_offset, correction_lowrank_first, correction_lowrank_second, correction_offset, gate_lowrank_first, gate_lowrank_second, key_rate_blend, self_token_scale, per_head_gain, per_head_bias, mixer_output_weight, mixer_norm_gain, mixer_norm_bias, expert_norm_gain, expert_norm_bias, routes, routing_weight, expert_gate_weight, expert_up_weight, expert_down_weight):
    receptance_rows = jnp.dot(tokens, receptance_matrix, preferred_element_type=jnp.float32)
    key_rows = jnp.dot(tokens, key_matrix, preferred_element_type=jnp.float32)
    value_rows = jnp.dot(tokens, value_matrix, preferred_element_type=jnp.float32)
    mixer_result, next_state = recurrent_readout(tokens, prior_state, receptance_rows, key_rows, value_rows, decay_lowrank_first, decay_lowrank_second, decay_channel_offset, correction_lowrank_first, correction_lowrank_second, correction_offset, gate_lowrank_first, gate_lowrank_second, key_rate_blend, self_token_scale, per_head_gain, per_head_bias)
    mixed = jnp.dot(mixer_result, mixer_output_weight, preferred_element_type=jnp.float32)
    hidden = layer_norm(tokens.astype(jnp.float32) + mixed, mixer_norm_gain, mixer_norm_bias).astype(jnp.bfloat16)
    model_width = hidden.shape[1]
    flat_ids = routes.reshape(-1).astype(jnp.int32)
    slot_total = flat_ids.shape[0]
    sort_order = jnp.argsort(flat_ids, stable=True).astype(jnp.int32)
    sorted_ids = flat_ids[sort_order]
    expert_ids = jnp.arange(EXPERTS, dtype=jnp.int32)
    counts = lax.optimization_barrier(jnp.sum((flat_ids[None, :] == expert_ids[:, None]).astype(jnp.int32), 1))
    starts = jnp.cumsum(counts) - counts
    column = jnp.arange(N_EP * CAP, dtype=jnp.int32)

    def one_expert(expert_item):
        gate_mat, up_mat, down_mat, first_slot, slot_count = expert_item
        row_index = sort_order[jnp.minimum(first_slot + column, slot_total - 1)]
        live = (column < slot_count).astype(jnp.bfloat16)
        rows_in = hidden[row_index // TOP] * live[:, None]
        gate_val = jnp.dot(rows_in, gate_mat, preferred_element_type=jnp.float32)
        up_val = jnp.dot(rows_in, up_mat, preferred_element_type=jnp.float32)
        inner = (jax.nn.silu(gate_val) * up_val).astype(jnp.bfloat16)
        return jnp.dot(inner, down_mat, preferred_element_type=jnp.float32).astype(jnp.bfloat16)
    produced = lax.map(one_expert, (expert_gate_weight, expert_up_weight, expert_down_weight, starts, counts))
    position = jnp.arange(slot_total, dtype=jnp.int32) - starts[sorted_ids]
    sorted_out = produced[sorted_ids, position]
    flat_out = jnp.zeros_like(sorted_out).at[sort_order].set(sorted_out)
    share = routing_weight / lax.optimization_barrier(jnp.sum(routing_weight, -1, keepdims=True))
    combined = lax.optimization_barrier(jnp.sum(flat_out.reshape(-1, TOP, model_width).astype(jnp.float32) * share[..., None], 1))
    result = layer_norm(hidden.astype(jnp.float32) + combined, expert_norm_gain, expert_norm_bias).astype(jnp.bfloat16)
    return (result, next_state)
```

```python
import functools

import jax
import jax.numpy as jnp
from jax import lax
from jax.experimental import pallas as pl
from jax.experimental.pallas import tpu as pltpu
from jax.sharding import PartitionSpec as P

F32 = jnp.float32
BF16 = jnp.bfloat16
MESH = pl.DeviceIdType.MESH
LANES = 128


def layer_norm(values_in, gain_vec, bias_vec):
    row_mean = jnp.mean(values_in, -1, keepdims=True)
    centered = values_in - row_mean
    row_var = jnp.mean(centered * centered, -1, keepdims=True)
    return centered * lax.rsqrt(row_var + 1e-05) * gain_vec + bias_vec


def matmul(left, right):
    return jnp.dot(left, right, preferred_element_type=F32)


def sigmoid(u):
    return 1.0 / (1.0 + jnp.exp(-u))


def kernel(
    n,
    capacity,
    routes,
    routing_weight,
    tokens_hbm,
    state_hbm,
    key_hbm,
    value_hbm,
    receptance_hbm,
    mixer_out_hbm,
    decay_first_hbm,
    decay_second_hbm,
    learn_first_hbm,
    learn_second_hbm,
    gate_first_hbm,
    gate_second_hbm,
    decay_offset_hbm,
    learn_offset_hbm,
    blend_hbm,
    head_gain_hbm,
    head_bias_hbm,
    mixer_gain_hbm,
    mixer_bias_hbm,
    expert_gain_hbm,
    expert_bias_hbm,
    self_scale_hbm,
    expert_gate_hbm,
    expert_up_hbm,
    expert_down_hbm,
    result,
    next_hbm,
    tokens,
    state,
    weights,
    decay_first,
    decay_second,
    learn_first,
    learn_second,
    gate_first,
    gate_second,
    vectors,
    self_scale,
    expert_gate,
    expert_up,
    expert_down,
    token_send,
    token_recv,
    part_send,
    part_recv,
    slot_send,
    slot_recv,
    back_send,
    back_recv,
    heads,
    value_flat,
    mixed_rows,
    load_sem,
    state_in_sem,
    state_out_sem,
    weight_sem,
    weight_send_sem,
    weight_recv_sem,
    token_send_sem,
    token_recv_sem,
    part_send_sem,
    part_recv_sem,
    slot_send_sem,
    slot_recv_sem,
    back_send_sem,
    back_recv_sem,
):
    me = lax.axis_index("ep")
    chips = n // 2
    chip, core = me // 2, lax.rem(me, 2)
    partner = chip * 2 + (1 - core)
    rows, width = tokens.shape
    head_count, head_size = self_scale.shape
    matrix_rows = key_hbm.shape[0]
    chip_rows = 2 * matrix_rows
    block = token_recv.shape[-1]

    if chip_rows < block:
        weights[...] = jnp.zeros_like(weights)

    barrier = pltpu.get_barrier_semaphore()

    def greet(step, carry):
        pl.semaphore_signal(
            barrier, inc=1, device_id={"ep": lax.rem(me + step, n)}, device_id_type=MESH
        )
        return carry

    lax.fori_loop(1, n, greet, 0)

    loads = [
        (tokens_hbm, tokens),
        (decay_first_hbm, decay_first),
        (learn_first_hbm, learn_first),
        (gate_first_hbm, gate_first),
        (decay_second_hbm, decay_second),
        (learn_second_hbm, learn_second),
        (gate_second_hbm, gate_second),
        (decay_offset_hbm, vectors.at[0]),
        (learn_offset_hbm, vectors.at[1]),
        (blend_hbm, vectors.at[2]),
        (head_gain_hbm, vectors.at[3]),
        (head_bias_hbm, vectors.at[4]),
        (mixer_gain_hbm, vectors.at[5]),
        (mixer_bias_hbm, vectors.at[6]),
        (expert_gain_hbm, vectors.at[7]),
        (expert_bias_hbm, vectors.at[8]),
        (self_scale_hbm, self_scale),
        (expert_gate_hbm.at[0], expert_gate),
        (expert_up_hbm.at[0], expert_up),
        (expert_down_hbm.at[0], expert_down),
    ]
    copies = [
        pltpu.make_async_copy(src, dst, load_sem.at[i]) for i, (src, dst) in enumerate(loads)
    ]
    row_at = pl.multiple_of(lax.rem(chip * chip_rows, block) + core * matrix_rows, matrix_rows)
    other_at = pl.multiple_of(
        lax.rem(chip * chip_rows, block) + (1 - core) * matrix_rows, matrix_rows
    )
    sources = (key_hbm, value_hbm, receptance_hbm, mixer_out_hbm)
    own_weight = [
        pltpu.make_async_copy(src, weights.at[i, pl.ds(row_at, matrix_rows), :], weight_sem.at[i])
        for i, src in enumerate(sources)
    ]
    push_weight = [
        pltpu.make_async_remote_copy(
            src_ref=src,
            dst_ref=weights.at[i, pl.ds(row_at, matrix_rows), :],
            send_sem=weight_send_sem.at[i],
            recv_sem=weight_recv_sem.at[i],
            device_id={"ep": partner},
            device_id_type=MESH,
        )
        for i, src in enumerate(sources)
    ]
    pull_weight = [
        pltpu.make_async_remote_copy(
            src_ref=src,
            dst_ref=weights.at[i, pl.ds(other_at, matrix_rows), :],
            send_sem=weight_send_sem.at[i],
            recv_sem=weight_recv_sem.at[i],
            device_id={"ep": partner},
            device_id_type=MESH,
        )
        for i, src in enumerate(sources)
    ]
    for copy in copies[:7]:
        copy.start()
    for copy in own_weight[:3]:
        copy.start()
    for copy in copies[7:17]:
        copy.start()
    state_in = [
        pltpu.make_async_copy(state_hbm.at[t], state.at[t], state_in_sem.at[t]) for t in range(rows)
    ]
    for copy in state_in:
        copy.start()
    own_weight[3].start()
    for copy in copies[17:]:
        copy.start()

    def chip_copy(send_ref, recv_ref, send_sem, recv_sem, to, source):
        return pltpu.make_async_remote_copy(
            src_ref=send_ref.at[to],
            dst_ref=recv_ref.at[source],
            send_sem=send_sem.at[to],
            recv_sem=recv_sem.at[source],
            device_id={"ep": to * 2 + core},
            device_id_type=MESH,
        )

    def device_copy(send_ref, recv_ref, send_sem, recv_sem, to, source):
        return pltpu.make_async_remote_copy(
            src_ref=send_ref.at[to],
            dst_ref=recv_ref.at[source],
            send_sem=send_sem.at[to],
            recv_sem=recv_sem.at[source],
            device_id={"ep": to},
            device_id_type=MESH,
        )

    def exchange(make, count, own):
        def send(step, carry):
            make(lax.rem(own + step, count), own).start()
            return carry

        def finish(step, carry):
            other = lax.rem(own + step, count)
            make(other, other).wait_recv()
            return carry

        def drain(step, carry):
            make(lax.rem(own + step, count), own).wait_send()
            return carry

        return (
            lambda: lax.fori_loop(1, count, send, 0),
            lambda: lax.fori_loop(1, count, finish, 0),
            lambda: lax.fori_loop(1, count, drain, 0),
        )

    def among_chips(send_ref, recv_ref, send_sem, recv_sem):
        return exchange(
            functools.partial(chip_copy, send_ref, recv_ref, send_sem, recv_sem), chips, chip
        )

    def among_devices(send_ref, recv_ref, send_sem, recv_sem):
        return exchange(
            functools.partial(device_copy, send_ref, recv_ref, send_sem, recv_sem), n, me
        )

    def spread(phase, flat):
        send_ref, recv_ref = token_send.at[phase], token_recv.at[phase]
        for j in range(chips):
            at = j * chip_rows // block * block
            send_ref[j] = flat[:, at : at + block]
        recv_ref[chip] = send_ref[chip]
        return among_chips(
            send_ref, recv_ref, token_send_sem.at[phase], token_recv_sem.at[phase]
        )

    def gathered(phase):
        return jnp.concatenate([token_recv[phase, j] for j in range(chips)], 0).astype(BF16)

    def partial_product(i, segment):
        own_weight[i].wait()
        pull_weight[i].wait_recv()
        product = matmul(segment, weights[i])
        for j in range(chips):
            part_send[i, j] = product[j * rows : (j + 1) * rows].astype(BF16)
        part_recv[i, chip] = part_send[i, chip]
        return among_chips(
            part_send.at[i], part_recv.at[i], part_send_sem.at[i], part_recv_sem.at[i]
        )

    def summed(i):
        total = part_recv[i, 0].astype(F32)
        for j in range(1, chips):
            total = total + part_recv[i, j].astype(F32)
        return total

    copies[0].wait()
    own = tokens[...]
    own_wide = own.astype(F32)
    token_go, token_wait, token_drain = spread(0, own_wide)
    pl.semaphore_wait(barrier, n - 1)
    token_go()
    for copy in push_weight:
        copy.start()

    for copy in copies[1:17]:
        copy.wait()
    squash = jnp.tanh(matmul(own, decay_first[...])).astype(BF16)
    pre_decay = vectors[0] + matmul(squash, decay_second[...])
    softplus = jnp.maximum(-pre_decay, 0.0) + jnp.log(1.0 + jnp.exp(-jnp.abs(pre_decay)))
    decay_rate = jnp.exp(-jnp.exp(-softplus - 0.5))
    low = matmul(own, learn_first[...]).astype(BF16)
    learn_rate = sigmoid(vectors[1] + matmul(low, learn_second[...]))
    key_factor = 1.0 + (learn_rate - 1.0) * vectors[2]
    opened = sigmoid(matmul(own, gate_first[...])).astype(BF16)
    gating = matmul(opened, gate_second[...])

    def by_head(i, flat):
        for h in range(head_count):
            heads[i, h * rows : (h + 1) * rows, :] = flat[:, h * head_size : (h + 1) * head_size]

    by_head(0, decay_rate)
    by_head(1, learn_rate)
    by_head(2, key_factor)

    token_wait()
    segment = gathered(0)
    parts = []
    for i in range(3):
        part = partial_product(i, segment)
        part[0]()
        parts.append(part)
    parts[0][1]()
    by_head(3, summed(0))
    parts[1][1]()
    value_flat[...] = summed(1)
    parts[2][1]()
    by_head(4, summed(2))

    mask_shape = (head_count, width)
    in_head = (
        lax.broadcasted_iota(jnp.int32, mask_shape, 1) // head_size
        == lax.broadcasted_iota(jnp.int32, mask_shape, 0)
    )
    for t in range(rows):
        decay_t, learn_t, factor_t, key_t, rec_t = [
            heads[i, pl.ds(t, head_count, stride=rows), :] for i in range(5)
        ]
        unit_t = key_t * lax.rsqrt(jnp.sum(key_t * key_t, -1, keepdims=True) + 1e-06)
        written_t = key_t * factor_t
        change_t = unit_t * learn_t
        value_t = jnp.broadcast_to(value_flat[t : t + 1, :], mask_shape)
        probes = jnp.concatenate([unit_t, decay_t * rec_t], 0).astype(BF16)
        state_in[t].wait()
        before = state[t]
        flat_state = before.reshape(width, head_size)
        found = lax.dot_general(
            probes, flat_state.astype(BF16), (((1,), (1,)), ((), ())), preferred_element_type=F32
        )
        removed = found[:head_count]
        change_rec = jnp.sum(change_t * rec_t, -1, keepdims=True)
        written_rec = jnp.sum(written_t * rec_t, -1, keepdims=True)
        own_term = jnp.sum(rec_t * written_t * self_scale[...], -1, keepdims=True)
        readout = jnp.where(
            in_head, found[head_count:] - removed * change_rec + value_t * written_rec, 0.0
        )
        head_mean = jnp.sum(readout, -1, keepdims=True) * (1.0 / head_size)
        head_dev = jnp.where(in_head, readout - head_mean, 0.0)
        head_var = jnp.sum(head_dev * head_dev, -1, keepdims=True) * (1.0 / head_size)
        normed = head_dev * lax.rsqrt(head_var + 0.00064)
        mixed_rows[t : t + 1, :] = jnp.sum(normed, 0, keepdims=True)
        mixed_rows[rows + t : rows + t + 1, :] = jnp.sum(
            jnp.where(in_head, own_term * value_t, 0.0), 0, keepdims=True
        )
        columns = jnp.concatenate(
            [jnp.where(in_head, value_t, 0.0), jnp.where(in_head, -removed, 0.0)], 0
        ).astype(BF16)
        rank_rows = jnp.concatenate([written_t, change_t], 0).astype(BF16)
        added = lax.dot_general(
            columns, rank_rows, (((0,), (0,)), ((), ())), preferred_element_type=F32
        ).reshape(head_count, head_size, head_size)
        for h in range(head_count):
            state[t, h] = before[h] * decay_t[h : h + 1, :] + added[h]
        pltpu.make_async_copy(state.at[t], next_hbm.at[t], state_out_sem.at[t]).start()

    normed = mixed_rows[:rows] * vectors[3] + vectors[4]
    mixer_result = ((normed + mixed_rows[rows:]) * gating).astype(BF16).astype(F32)
    mixer_go, mixer_wait, mixer_drain = spread(1, mixer_result)
    mixer_go()
    mixer_wait()
    out_go, out_wait, out_drain = partial_product(3, gathered(1))
    out_go()

    top = routes.shape[1]
    slots = n * capacity

    def routing(shape, axis):
        slot = lax.broadcasted_iota(jnp.int32, shape, axis)
        expert, place = slot // capacity, lax.rem(slot, capacity)
        earlier = jnp.zeros(shape, jnp.int32)
        held, shares = [], []
        for t in range(rows):
            hit = jnp.zeros(shape, jnp.int32)
            weight = jnp.zeros(shape, F32)
            total = jnp.zeros(shape, F32)
            for k in range(top):
                same = expert == routes[t, k]
                hit = hit + jnp.where(same, 1, 0)
                weight = weight + jnp.where(same, routing_weight[t, k], 0.0)
                total = total + routing_weight[t, k]
            live = (earlier == place) & (hit > 0)
            held.append(jnp.where(live, 1.0, 0.0))
            shares.append(jnp.where(live, weight / total, 0.0))
            earlier = earlier + hit
        return held, shares

    held, _ = routing((slots, 1), 0)
    _, shares = routing((1, slots), 1)
    share = jnp.concatenate(shares, 0)
    share_high = share.astype(BF16)
    share_low = (share - share_high.astype(F32)).astype(BF16)

    out_wait()
    hidden = (
        layer_norm(own_wide + summed(3), vectors[5], vectors[6]).astype(BF16).astype(F32)
    )
    outgoing = held[0] * hidden[0:1]
    for t in range(1, rows):
        outgoing = outgoing + held[t] * hidden[t : t + 1]
    for e in range(n):
        slot_send[e] = outgoing[e * capacity : (e + 1) * capacity].astype(BF16)
    slot_recv[me] = slot_send[me]
    slot_go, slot_wait, slot_drain = among_devices(
        slot_send, slot_recv, slot_send_sem, slot_recv_sem
    )
    slot_go()
    for copy in copies[17:]:
        copy.wait()
    slot_wait()
    arrived = jnp.concatenate([slot_recv[s].astype(F32) for s in range(n)], 0).astype(BF16)
    gate_val = matmul(arrived, expert_gate[...])
    up_val = matmul(arrived, expert_up[...])
    inner = (gate_val * sigmoid(gate_val) * up_val).astype(BF16)
    produced = matmul(inner, expert_down[...])
    for s in range(n):
        back_send[s] = produced[s * capacity : (s + 1) * capacity].astype(BF16)
    back_recv[me] = back_send[me]
    back_go, back_wait, back_drain = among_devices(
        back_send, back_recv, back_send_sem, back_recv_sem
    )
    back_go()
    token_drain()
    mixer_drain()
    for part in parts:
        part[2]()
    out_drain()
    slot_drain()
    for copy in push_weight:
        copy.wait_send()
    for t in range(rows):
        pltpu.make_async_copy(state.at[t], next_hbm.at[t], state_out_sem.at[t]).wait()
    back_wait()
    returned = jnp.concatenate([back_recv[e].astype(F32) for e in range(n)], 0).astype(BF16)
    combined = matmul(share_high, returned) + matmul(share_low, returned)
    result[...] = layer_norm(hidden + combined, vectors[7], vectors[8]).astype(BF16)
    back_drain()


def body(
    tokens,
    prior_state,
    receptance_matrix,
    key_matrix,
    value_matrix,
    decay_lowrank_first,
    decay_lowrank_second,
    decay_channel_offset,
    correction_lowrank_first,
    correction_lowrank_second,
    correction_offset,
    gate_lowrank_first,
    gate_lowrank_second,
    key_rate_blend,
    self_token_scale,
    per_head_gain,
    per_head_bias,
    mixer_output_weight,
    mixer_norm_gain,
    mixer_norm_bias,
    expert_norm_gain,
    expert_norm_bias,
    routes,
    routing_weight,
    expert_gate_weight,
    expert_up_weight,
    expert_down_weight,
):
    n = lax.axis_size("ep")
    chips = n // 2
    rows, width = tokens.shape
    head_count, head_size = self_token_scale.shape
    capacity = max(2, 2 * rows * routes.shape[1] // n)
    block = max(2 * key_matrix.shape[0], LANES)
    vectors = [
        v.reshape(1, -1)
        for v in (
            decay_channel_offset,
            correction_offset,
            key_rate_blend,
            per_head_gain,
            per_head_bias,
            mixer_norm_gain,
            mixer_norm_bias,
            expert_norm_gain,
            expert_norm_bias,
        )
    ]
    anywhere = pl.BlockSpec(memory_space=pl.ANY)
    scalars = pl.BlockSpec(memory_space=pltpu.SMEM)
    dma = pltpu.SemaphoreType.DMA
    vmem = pltpu.VMEM
    operands = [
        tokens,
        prior_state,
        key_matrix,
        value_matrix,
        receptance_matrix,
        mixer_output_weight,
        decay_lowrank_first,
        decay_lowrank_second,
        correction_lowrank_first,
        correction_lowrank_second,
        gate_lowrank_first,
        gate_lowrank_second,
        *vectors,
        self_token_scale,
        expert_gate_weight,
        expert_up_weight,
        expert_down_weight,
    ]
    return tuple(
        pl.pallas_call(
            functools.partial(kernel, n, capacity),
            out_shape=(
                jax.ShapeDtypeStruct(tokens.shape, BF16),
                jax.ShapeDtypeStruct(prior_state.shape, F32),
            ),
            in_specs=[scalars, scalars] + [anywhere] * len(operands),
            out_specs=(pl.BlockSpec(memory_space=pltpu.VMEM), anywhere),
            scratch_shapes=[
                vmem(tokens.shape, BF16),
                vmem(prior_state.shape, F32),
                vmem((4, block, width), BF16),
                vmem(decay_lowrank_first.shape, BF16),
                vmem(decay_lowrank_second.shape, BF16),
                vmem(correction_lowrank_first.shape, BF16),
                vmem(correction_lowrank_second.shape, BF16),
                vmem(gate_lowrank_first.shape, BF16),
                vmem(gate_lowrank_second.shape, BF16),
                vmem((len(vectors), 1, width), F32),
                vmem(self_token_scale.shape, F32),
                vmem(expert_gate_weight.shape[1:], BF16),
                vmem(expert_up_weight.shape[1:], BF16),
                vmem(expert_down_weight.shape[1:], BF16),
                vmem((2, chips, rows, block), F32),
                vmem((2, chips, rows, block), F32),
                vmem((4, chips, rows, width), BF16),
                vmem((4, chips, rows, width), BF16),
                vmem((n, capacity, width), BF16),
                vmem((n, capacity, width), BF16),
                vmem((n, capacity, width), BF16),
                vmem((n, capacity, width), BF16),
                vmem((5, head_count * rows, head_size), F32),
                vmem((rows, width), F32),
                vmem((2 * rows, width), F32),
                dma((20,)),
                dma((rows,)),
                dma((rows,)),
                dma((4,)),
                dma((4,)),
                dma((4,)),
                dma((2, chips)),
                dma((2, chips)),
                dma((4, chips)),
                dma((4, chips)),
                dma((n,)),
                dma((n,)),
                dma((n,)),
                dma((n,)),
            ],
            compiler_params=pltpu.CompilerParams(
                collective_id=0, has_side_effects=True, vmem_limit_bytes=60 * 1024 * 1024
            ),
        )(routes, routing_weight, *operands)
    )


def solution(mesh):
    split = P(("grp", "ep"), None)
    state = P(("grp", "ep"), None, None, None)
    matrix = P("ep", None)
    expert = P("ep", None, None)
    in_specs = (
        (split, state)
        + (matrix,) * 3
        + (P(),) * 12
        + (matrix,)
        + (P(),) * 4
        + (split, split)
        + (expert,) * 3
    )
    return jax.shard_map(
        body, mesh=mesh, in_specs=in_specs, out_specs=(split, state), check_vma=False
    )
```

```python
import functools

import jax
import jax.numpy as jnp
from jax import lax
from jax.experimental import pallas as pl
from jax.experimental.pallas import tpu as pltpu
from jax.sharding import PartitionSpec as P

F32 = jnp.float32
BF16 = jnp.bfloat16
MESH = pl.DeviceIdType.MESH
LANES = 128


def layer_norm(values_in, gain_vec, bias_vec):
    row_mean = jnp.mean(values_in, -1, keepdims=True)
    centered = values_in - row_mean
    row_var = jnp.mean(centered * centered, -1, keepdims=True)
    return centered * lax.rsqrt(row_var + 1e-05) * gain_vec + bias_vec


def matmul(left, right):
    return jnp.dot(left, right, preferred_element_type=F32)


def matmul_t(left, right):
    return lax.dot_general(left, right, (((1,), (1,)), ((), ())), preferred_element_type=F32)


def sigmoid(u):
    return 1.0 / (1.0 + jnp.exp(-u))


def kernel(
    n,
    capacity,
    routes,
    routing_weight,
    tokens_hbm,
    state_hbm,
    key_hbm,
    value_hbm,
    receptance_hbm,
    mixer_out_hbm,
    decay_first_hbm,
    decay_second_hbm,
    learn_first_hbm,
    learn_second_hbm,
    gate_first_hbm,
    gate_second_hbm,
    decay_offset_hbm,
    learn_offset_hbm,
    blend_hbm,
    head_gain_hbm,
    head_bias_hbm,
    mixer_gain_hbm,
    mixer_bias_hbm,
    self_scale_hbm,
    expert_gate_hbm,
    expert_up_hbm,
    expert_down_hbm,
    next_state,
    returned,
    hidden_out,
    share_out,
    tokens,
    state,
    weights,
    decay_first,
    decay_second,
    learn_first,
    learn_second,
    gate_first,
    gate_second,
    vectors,
    self_scale,
    expert_gate,
    expert_up,
    expert_down,
    token_send,
    token_recv,
    part_send,
    part_recv,
    slot_send,
    slot_recv,
    back_send,
    heads,
    value_flat,
    mixed_rows,
    columns,
    rank_rows,
    back_recv,
    load_sem,
    state_in_sem,
    weight_sem,
    weight_send_sem,
    weight_recv_sem,
    token_send_sem,
    token_recv_sem,
    part_send_sem,
    part_recv_sem,
    slot_send_sem,
    slot_recv_sem,
    back_send_sem,
    back_recv_sem,
):
    me = lax.axis_index("ep")
    chips = n // 2
    chip, core = me // 2, lax.rem(me, 2)
    partner = chip * 2 + (1 - core)
    rows, width = tokens.shape
    head_count, head_size = self_scale.shape
    matrix_rows = key_hbm.shape[0]
    chip_rows = 2 * matrix_rows
    block = token_recv.shape[-1]

    if chip_rows < block:
        weights[...] = jnp.zeros_like(weights)

    barrier = pltpu.get_barrier_semaphore()

    def greet(step, carry):
        pl.semaphore_signal(
            barrier, inc=1, device_id={"ep": lax.rem(me + step, n)}, device_id_type=MESH
        )
        return carry

    lax.fori_loop(1, n, greet, 0)

    loads = [
        (tokens_hbm, tokens),
        (decay_first_hbm, decay_first),
        (learn_first_hbm, learn_first),
        (gate_first_hbm, gate_first),
        (decay_second_hbm, decay_second),
        (learn_second_hbm, learn_second),
        (gate_second_hbm, gate_second),
        (decay_offset_hbm, vectors.at[0]),
        (learn_offset_hbm, vectors.at[1]),
        (blend_hbm, vectors.at[2]),
        (head_gain_hbm, vectors.at[3]),
        (head_bias_hbm, vectors.at[4]),
        (mixer_gain_hbm, vectors.at[5]),
        (mixer_bias_hbm, vectors.at[6]),
        (self_scale_hbm, self_scale),
        (expert_gate_hbm.at[0], expert_gate),
        (expert_up_hbm.at[0], expert_up),
        (expert_down_hbm.at[0], expert_down),
    ]
    copies = [
        pltpu.make_async_copy(src, dst, load_sem.at[i]) for i, (src, dst) in enumerate(loads)
    ]
    row_at = pl.multiple_of(lax.rem(chip * chip_rows, block) + core * matrix_rows, matrix_rows)
    other_at = pl.multiple_of(
        lax.rem(chip * chip_rows, block) + (1 - core) * matrix_rows, matrix_rows
    )
    sources = (key_hbm, value_hbm, receptance_hbm, mixer_out_hbm)
    own_weight = [
        pltpu.make_async_copy(src, weights.at[i, pl.ds(row_at, matrix_rows), :], weight_sem.at[i])
        for i, src in enumerate(sources)
    ]
    push_weight = [
        pltpu.make_async_remote_copy(
            src_ref=src,
            dst_ref=weights.at[i, pl.ds(row_at, matrix_rows), :],
            send_sem=weight_send_sem.at[i],
            recv_sem=weight_recv_sem.at[i],
            device_id={"ep": partner},
            device_id_type=MESH,
        )
        for i, src in enumerate(sources)
    ]
    pull_weight = [
        pltpu.make_async_remote_copy(
            src_ref=src,
            dst_ref=weights.at[i, pl.ds(other_at, matrix_rows), :],
            send_sem=weight_send_sem.at[i],
            recv_sem=weight_recv_sem.at[i],
            device_id={"ep": partner},
            device_id_type=MESH,
        )
        for i, src in enumerate(sources)
    ]
    for copy in copies[:7]:
        copy.start()
    for copy in own_weight[:3]:
        copy.start()
    for copy in copies[7:15]:
        copy.start()
    state_in = [
        pltpu.make_async_copy(state_hbm.at[t], state.at[t], state_in_sem.at[t]) for t in range(rows)
    ]
    for copy in state_in:
        copy.start()
    own_weight[3].start()
    for copy in copies[15:]:
        copy.start()

    def chip_copy(send_ref, recv_ref, send_sem, recv_sem, to, source):
        return pltpu.make_async_remote_copy(
            src_ref=send_ref.at[to],
            dst_ref=recv_ref.at[source],
            send_sem=send_sem.at[to],
            recv_sem=recv_sem.at[source],
            device_id={"ep": to * 2 + core},
            device_id_type=MESH,
        )

    def device_copy(send_ref, recv_ref, send_sem, recv_sem, to, source):
        return pltpu.make_async_remote_copy(
            src_ref=send_ref.at[to],
            dst_ref=recv_ref.at[source],
            send_sem=send_sem.at[to],
            recv_sem=recv_sem.at[source],
            device_id={"ep": to},
            device_id_type=MESH,
        )

    def exchange(make, count, own):
        def send(step, carry):
            make(lax.rem(own + step, count), own).start()
            return carry

        def finish(step, carry):
            other = lax.rem(own + step, count)
            make(other, other).wait_recv()
            return carry

        def drain(step, carry):
            make(lax.rem(own + step, count), own).wait_send()
            return carry

        return (
            lambda: lax.fori_loop(1, count, send, 0),
            lambda: lax.fori_loop(1, count, finish, 0),
            lambda: lax.fori_loop(1, count, drain, 0),
        )

    def among_chips(send_ref, recv_ref, send_sem, recv_sem):
        return exchange(
            functools.partial(chip_copy, send_ref, recv_ref, send_sem, recv_sem), chips, chip
        )

    def among_devices(send_ref, recv_ref, send_sem, recv_sem):
        return exchange(
            functools.partial(device_copy, send_ref, recv_ref, send_sem, recv_sem), n, me
        )

    def spread(phase, flat):
        send_ref, recv_ref = token_send.at[phase], token_recv.at[phase]
        for j in range(chips):
            at = j * chip_rows // block * block
            send_ref[j] = flat[:, at : at + block]
        recv_ref[chip] = send_ref[chip]
        return among_chips(
            send_ref, recv_ref, token_send_sem.at[phase], token_recv_sem.at[phase]
        )

    def gathered(phase):
        return jnp.concatenate([token_recv[phase, j] for j in range(chips)], 0).astype(BF16)

    def partial_product(i, segment):
        own_weight[i].wait()
        pull_weight[i].wait_recv()
        product = matmul(segment, weights[i])
        for j in range(chips):
            part_send[i, j] = product[j * rows : (j + 1) * rows].astype(BF16)
        part_recv[i, chip] = part_send[i, chip]
        return among_chips(
            part_send.at[i], part_recv.at[i], part_send_sem.at[i], part_recv_sem.at[i]
        )

    def summed(i):
        total = part_recv[i, 0].astype(F32)
        for j in range(1, chips):
            total = total + part_recv[i, j].astype(F32)
        return total

    copies[0].wait()
    own = tokens[...]
    own_wide = own.astype(F32)
    token_go, token_wait, token_drain = spread(0, own_wide)
    pl.semaphore_wait(barrier, n - 1)
    token_go()
    for copy in push_weight:
        copy.start()

    for copy in copies[1:15]:
        copy.wait()
    squash = jnp.tanh(matmul_t(own, decay_first[...])).astype(BF16)
    pre_decay = vectors[0] + matmul(squash, decay_second[...])
    softplus = jnp.maximum(-pre_decay, 0.0) + jnp.log(1.0 + jnp.exp(-jnp.abs(pre_decay)))
    decay_rate = jnp.exp(-jnp.exp(-softplus - 0.5))
    low = matmul_t(own, learn_first[...]).astype(BF16)
    learn_rate = sigmoid(vectors[1] + matmul(low, learn_second[...]))
    key_factor = 1.0 + (learn_rate - 1.0) * vectors[2]
    opened = sigmoid(matmul(own, gate_first[...])).astype(BF16)
    gating = matmul(opened, gate_second[...])

    def by_head(i, flat):
        for h in range(head_count):
            heads[i, h * rows : (h + 1) * rows, :] = flat[:, h * head_size : (h + 1) * head_size]

    by_head(0, decay_rate)
    by_head(1, learn_rate)
    by_head(2, key_factor)

    token_wait()
    segment = gathered(0)
    parts = []
    for i in range(3):
        part = partial_product(i, segment)
        part[0]()
        parts.append(part)
    parts[0][1]()
    by_head(3, summed(0))
    parts[1][1]()
    value_flat[...] = summed(1)
    parts[2][1]()
    by_head(4, summed(2))

    mask_shape = (head_count, width)
    in_head = (
        lax.broadcasted_iota(jnp.int32, mask_shape, 1) // head_size
        == lax.broadcasted_iota(jnp.int32, mask_shape, 0)
    )
    for t in range(rows):
        decay_t, learn_t, factor_t, key_t, rec_t = [
            heads[i, pl.ds(t, head_count, stride=rows), :] for i in range(5)
        ]
        unit_t = key_t * lax.rsqrt(jnp.sum(key_t * key_t, -1, keepdims=True) + 1e-06)
        written_t = key_t * factor_t
        change_t = unit_t * learn_t
        value_t = jnp.broadcast_to(value_flat[t : t + 1, :], mask_shape)
        probes = jnp.concatenate([unit_t, decay_t * rec_t], 0).astype(BF16)
        state_in[t].wait()
        before = state[t]
        flat_state = before.reshape(width, head_size)
        found = lax.dot_general(
            probes, flat_state.astype(BF16), (((1,), (1,)), ((), ())), preferred_element_type=F32
        )
        removed = found[:head_count]
        change_rec = jnp.sum(change_t * rec_t, -1, keepdims=True)
        written_rec = jnp.sum(written_t * rec_t, -1, keepdims=True)
        own_term = jnp.sum(rec_t * written_t * self_scale[...], -1, keepdims=True)
        readout = jnp.where(
            in_head, found[head_count:] - removed * change_rec + value_t * written_rec, 0.0
        )
        head_mean = jnp.sum(readout, -1, keepdims=True) * (1.0 / head_size)
        head_dev = jnp.where(in_head, readout - head_mean, 0.0)
        head_var = jnp.sum(head_dev * head_dev, -1, keepdims=True) * (1.0 / head_size)
        normed = head_dev * lax.rsqrt(head_var + 0.00064)
        mixed_rows[t : t + 1, :] = jnp.sum(normed, 0, keepdims=True)
        mixed_rows[rows + t : rows + t + 1, :] = jnp.sum(
            jnp.where(in_head, own_term * value_t, 0.0), 0, keepdims=True
        )
        columns[t] = jnp.concatenate(
            [jnp.where(in_head, value_t, 0.0), jnp.where(in_head, -removed, 0.0)], 0
        ).astype(BF16)
        rank_rows[t] = jnp.concatenate([written_t, change_t], 0).astype(BF16)

    normed = mixed_rows[:rows] * vectors[3] + vectors[4]
    mixer_result = ((normed + mixed_rows[rows:]) * gating).astype(BF16).astype(F32)
    mixer_go, mixer_wait, mixer_drain = spread(1, mixer_result)
    mixer_go()
    for t in range(rows):
        decay_t = heads[0, pl.ds(t, head_count, stride=rows), :]
        added = lax.dot_general(
            columns[t], rank_rows[t], (((0,), (0,)), ((), ())), preferred_element_type=F32
        ).reshape(head_count, head_size, head_size)
        for h in range(head_count):
            next_state[t, h] = state[t, h] * decay_t[h : h + 1, :] + added[h]
    mixer_wait()
    out_go, out_wait, out_drain = partial_product(3, gathered(1))
    out_go()

    top = routes.shape[1]
    slots = n * capacity

    def routing(shape, axis):
        slot = lax.broadcasted_iota(jnp.int32, shape, axis)
        expert, place = slot // capacity, lax.rem(slot, capacity)
        earlier = jnp.zeros(shape, jnp.int32)
        held, shares = [], []
        for t in range(rows):
            hit = jnp.zeros(shape, jnp.int32)
            weight = jnp.zeros(shape, F32)
            total = jnp.zeros(shape, F32)
            for k in range(top):
                same = expert == routes[t, k]
                hit = hit + jnp.where(same, 1, 0)
                weight = weight + jnp.where(same, routing_weight[t, k], 0.0)
                total = total + routing_weight[t, k]
            live = (earlier == place) & (hit > 0)
            held.append(jnp.where(live, 1.0, 0.0))
            shares.append(jnp.where(live, weight / total, 0.0))
            earlier = earlier + hit
        return held, shares

    held, _ = routing((slots, 1), 0)
    _, shares = routing((1, slots), 1)
    share_out[...] = jnp.concatenate(shares, 0)

    out_wait()
    hidden = (
        layer_norm(own_wide + summed(3), vectors[5], vectors[6]).astype(BF16).astype(F32)
    )
    hidden_out[...] = hidden
    outgoing = held[0] * hidden[0:1]
    for t in range(1, rows):
        outgoing = outgoing + held[t] * hidden[t : t + 1]
    for e in range(n):
        slot_send[e] = outgoing[e * capacity : (e + 1) * capacity].astype(BF16)
    slot_recv[me] = slot_send[me]
    slot_go, slot_wait, slot_drain = among_devices(
        slot_send, slot_recv, slot_send_sem, slot_recv_sem
    )
    slot_go()
    for copy in copies[15:]:
        copy.wait()
    slot_wait()
    arrived = jnp.concatenate([slot_recv[s].astype(F32) for s in range(n)], 0).astype(BF16)
    gate_val = matmul(arrived, expert_gate[...])
    up_val = matmul(arrived, expert_up[...])
    inner = (gate_val * sigmoid(gate_val) * up_val).astype(BF16)
    produced = matmul(inner, expert_down[...])
    for s in range(n):
        back_send[s] = produced[s * capacity : (s + 1) * capacity].astype(BF16)
    back_recv[me] = back_send[me]
    back_go, back_wait, back_drain = among_devices(
        back_send, back_recv, back_send_sem, back_recv_sem
    )
    back_go()
    token_drain()
    mixer_drain()
    for part in parts:
        part[2]()
    out_drain()
    slot_drain()
    for copy in push_weight:
        copy.wait_send()
    back_wait()
    returned[...] = back_recv[...]
    back_drain()


def finish_kernel(
    state, returned, hidden, share, gain_hbm, bias_hbm, result_hbm, next_hbm, norm, result, sems
):
    rows = state.shape[0]
    copies = [
        pltpu.make_async_copy(gain_hbm, norm.at[0], sems.at[0]),
        pltpu.make_async_copy(bias_hbm, norm.at[1], sems.at[1]),
    ] + [
        pltpu.make_async_copy(state.at[t], next_hbm.at[t], sems.at[2 + t]) for t in range(rows)
    ]
    for copy in copies:
        copy.start()
    share_high = share[...].astype(BF16)
    share_low = (share[...] - share_high.astype(F32)).astype(BF16)
    rows_back = jnp.concatenate(
        [returned[e].astype(F32) for e in range(returned.shape[0])], 0
    ).astype(BF16)
    combined = matmul(share_high, rows_back) + matmul(share_low, rows_back)
    for copy in copies[:2]:
        copy.wait()
    result[...] = layer_norm(hidden[...] + combined, norm[0], norm[1]).astype(BF16)
    last = pltpu.make_async_copy(result, result_hbm, sems.at[2 + rows])
    last.start()
    for copy in copies[2:]:
        copy.wait()
    last.wait()


def body(
    tokens,
    prior_state,
    receptance_matrix,
    key_matrix,
    value_matrix,
    decay_lowrank_first,
    decay_lowrank_second,
    decay_channel_offset,
    correction_lowrank_first,
    correction_lowrank_second,
    correction_offset,
    gate_lowrank_first,
    gate_lowrank_second,
    key_rate_blend,
    self_token_scale,
    per_head_gain,
    per_head_bias,
    mixer_output_weight,
    mixer_norm_gain,
    mixer_norm_bias,
    expert_norm_gain,
    expert_norm_bias,
    routes,
    routing_weight,
    expert_gate_weight,
    expert_up_weight,
    expert_down_weight,
):
    n = lax.axis_size("ep")
    chips = n // 2
    rows, width = tokens.shape
    head_count, head_size = self_token_scale.shape
    capacity = max(2, 2 * rows * routes.shape[1] // n)
    block = max(2 * key_matrix.shape[0], LANES)
    vectors = [
        v.reshape(1, -1)
        for v in (
            decay_channel_offset,
            correction_offset,
            key_rate_blend,
            per_head_gain,
            per_head_bias,
            mixer_norm_gain,
            mixer_norm_bias,
            expert_norm_gain,
            expert_norm_bias,
        )
    ]
    decay_first, learn_first = decay_lowrank_first.T, correction_lowrank_first.T
    anywhere = pl.BlockSpec(memory_space=pltpu.HBM)
    scalars = pl.BlockSpec(memory_space=pltpu.SMEM)
    dma = pltpu.SemaphoreType.DMA
    vmem = pltpu.VMEM
    operands = [
        tokens,
        prior_state,
        key_matrix,
        value_matrix,
        receptance_matrix,
        mixer_output_weight,
        decay_first,
        decay_lowrank_second,
        learn_first,
        correction_lowrank_second,
        gate_lowrank_first,
        gate_lowrank_second,
        *vectors[:7],
        self_token_scale,
        expert_gate_weight,
        expert_up_weight,
        expert_down_weight,
    ]
    passed = pl.pallas_call(
            functools.partial(kernel, n, capacity),
            out_shape=(
                pltpu.VMEM(prior_state.shape, F32),
                pltpu.VMEM((n, capacity, width), BF16),
                pltpu.VMEM(tokens.shape, F32),
                pltpu.VMEM((rows, n * capacity), F32),
            ),
            in_specs=[scalars, scalars] + [anywhere] * len(operands),
            out_specs=(pl.BlockSpec(memory_space=pltpu.VMEM),) * 4,
            scratch_shapes=[
                vmem(tokens.shape, BF16),
                vmem(prior_state.shape, F32),
                vmem((4, block, width), BF16),
                vmem(decay_first.shape, BF16),
                vmem(decay_lowrank_second.shape, BF16),
                vmem(learn_first.shape, BF16),
                vmem(correction_lowrank_second.shape, BF16),
                vmem(gate_lowrank_first.shape, BF16),
                vmem(gate_lowrank_second.shape, BF16),
                vmem((7, 1, width), F32),
                vmem(self_token_scale.shape, F32),
                vmem(expert_gate_weight.shape[1:], BF16),
                vmem(expert_up_weight.shape[1:], BF16),
                vmem(expert_down_weight.shape[1:], BF16),
                vmem((2, chips, rows, block), F32),
                vmem((2, chips, rows, block), F32),
                vmem((4, chips, rows, width), BF16),
                vmem((4, chips, rows, width), BF16),
                vmem((n, capacity, width), BF16),
                vmem((n, capacity, width), BF16),
                vmem((n, capacity, width), BF16),
                vmem((5, head_count * rows, head_size), F32),
                vmem((rows, width), F32),
                vmem((2 * rows, width), F32),
                vmem((rows, 2 * head_count, width), BF16),
                vmem((rows, 2 * head_count, head_size), BF16),
                vmem((n, capacity, width), BF16),
                dma((18,)),
                dma((rows,)),
                dma((4,)),
                dma((4,)),
                dma((4,)),
                dma((2, chips)),
                dma((2, chips)),
                dma((4, chips)),
                dma((4, chips)),
                dma((n,)),
                dma((n,)),
                dma((n,)),
                dma((n,)),
            ],
            compiler_params=pltpu.CompilerParams(
                collective_id=0, has_side_effects=True, vmem_limit_bytes=52 * 1024 * 1024
            ),
        )(routes, routing_weight, *operands)
    inside = pl.BlockSpec(memory_space=pltpu.VMEM)
    return tuple(
        pl.pallas_call(
            finish_kernel,
            out_shape=(
                jax.ShapeDtypeStruct(tokens.shape, BF16),
                jax.ShapeDtypeStruct(prior_state.shape, F32),
            ),
            in_specs=[inside] * 4 + [anywhere] * 2,
            out_specs=(anywhere, anywhere),
            scratch_shapes=[
                vmem((2, 1, width), F32),
                vmem(tokens.shape, BF16),
                dma((rows + 3,)),
            ],
            compiler_params=pltpu.CompilerParams(vmem_limit_bytes=16 * 1024 * 1024),
        )(*passed, *vectors[7:])
    )


def solution(mesh):
    split = P(("grp", "ep"), None)
    state = P(("grp", "ep"), None, None, None)
    matrix = P("ep", None)
    expert = P("ep", None, None)
    in_specs = (
        (split, state)
        + (matrix,) * 3
        + (P(),) * 12
        + (matrix,)
        + (P(),) * 4
        + (split, split)
        + (expert,) * 3
    )
    return jax.shard_map(
        body, mesh=mesh, in_specs=in_specs, out_specs=(split, state), check_vma=False
    )
```

```python
import functools

import jax
import jax.numpy as jnp
from jax import lax
from jax.experimental import pallas as pl
from jax.experimental.pallas import tpu as pltpu
from jax.sharding import PartitionSpec as P

F32 = jnp.float32
BF16 = jnp.bfloat16
MESH = pl.DeviceIdType.MESH
LANES = 128


def layer_norm(values_in, gain_vec, bias_vec):
    row_mean = jnp.mean(values_in, -1, keepdims=True)
    centered = values_in - row_mean
    row_var = jnp.mean(centered * centered, -1, keepdims=True)
    return centered * lax.rsqrt(row_var + 1e-05) * gain_vec + bias_vec


def matmul(left, right):
    return jnp.dot(left, right, preferred_element_type=F32)


def matmul_t(left, right):
    return lax.dot_general(left, right, (((1,), (1,)), ((), ())), preferred_element_type=F32)


def sigmoid(u):
    return 1.0 / (1.0 + jnp.exp(-u))


def kernel(
    n,
    capacity,
    routes,
    routing_weight,
    tokens_hbm,
    state_hbm,
    key_hbm,
    value_hbm,
    receptance_hbm,
    mixer_out_hbm,
    decay_first_hbm,
    decay_second_hbm,
    learn_first_hbm,
    learn_second_hbm,
    gate_first_hbm,
    gate_second_hbm,
    decay_offset_hbm,
    learn_offset_hbm,
    blend_hbm,
    head_gain_hbm,
    head_bias_hbm,
    mixer_gain_hbm,
    mixer_bias_hbm,
    self_scale_hbm,
    expert_gate_hbm,
    expert_up_hbm,
    expert_down_hbm,
    next_state,
    returned,
    hidden_out,
    share_out,
    tokens,
    state,
    weights,
    decay_first,
    decay_second,
    learn_first,
    learn_second,
    gate_first,
    gate_second,
    vectors,
    self_scale,
    expert_gate,
    expert_up,
    expert_down,
    token_send,
    token_recv,
    part_send,
    part_recv,
    slot_send,
    slot_recv,
    back_send,
    heads,
    value_flat,
    mixed_rows,
    columns,
    rank_rows,
    back_recv,
    load_sem,
    state_in_sem,
    weight_sem,
    weight_send_sem,
    weight_recv_sem,
    token_send_sem,
    token_recv_sem,
    part_send_sem,
    part_recv_sem,
    slot_send_sem,
    slot_recv_sem,
    back_send_sem,
    back_recv_sem,
):
    me = lax.axis_index("ep")
    chips = n // 2
    chip, core = me // 2, lax.rem(me, 2)
    partner = chip * 2 + (1 - core)
    rows, width = tokens.shape
    head_count, head_size = self_scale.shape
    matrix_rows = key_hbm.shape[0]
    chip_rows = 2 * matrix_rows
    block = token_recv.shape[-1]

    if chip_rows < block:
        weights[...] = jnp.zeros_like(weights)

    barrier = pltpu.get_barrier_semaphore()

    def greet(step, carry):
        pl.semaphore_signal(
            barrier, inc=1, device_id={"ep": lax.rem(me + step, n)}, device_id_type=MESH
        )
        return carry

    lax.fori_loop(1, n, greet, 0)

    loads = [
        (tokens_hbm, tokens),
        (decay_first_hbm, decay_first),
        (learn_first_hbm, learn_first),
        (gate_first_hbm, gate_first),
        (decay_second_hbm, decay_second),
        (learn_second_hbm, learn_second),
        (gate_second_hbm, gate_second),
        (decay_offset_hbm, vectors.at[0]),
        (learn_offset_hbm, vectors.at[1]),
        (blend_hbm, vectors.at[2]),
        (head_gain_hbm, vectors.at[3]),
        (head_bias_hbm, vectors.at[4]),
        (mixer_gain_hbm, vectors.at[5]),
        (mixer_bias_hbm, vectors.at[6]),
        (self_scale_hbm, self_scale),
        (expert_gate_hbm.at[0], expert_gate),
        (expert_up_hbm.at[0], expert_up),
        (expert_down_hbm.at[0], expert_down),
    ]
    copies = [
        pltpu.make_async_copy(src, dst, load_sem.at[i]) for i, (src, dst) in enumerate(loads)
    ]
    row_at = pl.multiple_of(lax.rem(chip * chip_rows, block) + core * matrix_rows, matrix_rows)
    other_at = pl.multiple_of(
        lax.rem(chip * chip_rows, block) + (1 - core) * matrix_rows, matrix_rows
    )
    sources = (key_hbm, value_hbm, receptance_hbm, mixer_out_hbm)
    own_weight = [
        pltpu.make_async_copy(src, weights.at[i, pl.ds(row_at, matrix_rows), :], weight_sem.at[i])
        for i, src in enumerate(sources)
    ]
    push_weight = [
        pltpu.make_async_remote_copy(
            src_ref=src,
            dst_ref=weights.at[i, pl.ds(row_at, matrix_rows), :],
            send_sem=weight_send_sem.at[i],
            recv_sem=weight_recv_sem.at[i],
            device_id={"ep": partner},
            device_id_type=MESH,
        )
        for i, src in enumerate(sources)
    ]
    pull_weight = [
        pltpu.make_async_remote_copy(
            src_ref=src,
            dst_ref=weights.at[i, pl.ds(other_at, matrix_rows), :],
            send_sem=weight_send_sem.at[i],
            recv_sem=weight_recv_sem.at[i],
            device_id={"ep": partner},
            device_id_type=MESH,
        )
        for i, src in enumerate(sources)
    ]
    for copy in copies[:7]:
        copy.start()
    for copy in own_weight[:3]:
        copy.start()
    for copy in copies[7:15]:
        copy.start()
    state_in = [
        pltpu.make_async_copy(state_hbm.at[t], state.at[t], state_in_sem.at[t]) for t in range(rows)
    ]
    for copy in state_in:
        copy.start()
    own_weight[3].start()
    for copy in copies[15:]:
        copy.start()

    def chip_copy(send_ref, recv_ref, send_sem, recv_sem, to, source):
        return pltpu.make_async_remote_copy(
            src_ref=send_ref.at[to],
            dst_ref=recv_ref.at[source],
            send_sem=send_sem.at[to],
            recv_sem=recv_sem.at[source],
            device_id={"ep": to * 2 + core},
            device_id_type=MESH,
        )

    def device_copy(send_ref, recv_ref, send_sem, recv_sem, to, source):
        return pltpu.make_async_remote_copy(
            src_ref=send_ref.at[to],
            dst_ref=recv_ref.at[source],
            send_sem=send_sem.at[to],
            recv_sem=recv_sem.at[source],
            device_id={"ep": to},
            device_id_type=MESH,
        )

    def exchange(make, count, own):
        def send(step, carry):
            away = (step + 1) // 2
            offset = count // 2 + away * (2 * lax.rem(step, 2) - 1)
            make(lax.rem(own + offset, count), own).start()
            return carry

        def finish(step, carry):
            other = lax.rem(own + step, count)
            make(other, other).wait_recv()
            return carry

        def drain(step, carry):
            make(lax.rem(own + step, count), own).wait_send()
            return carry

        return (
            lambda: lax.fori_loop(0, count - 1, send, 0),
            lambda: lax.fori_loop(1, count, finish, 0),
            lambda: lax.fori_loop(1, count, drain, 0),
        )

    def among_chips(send_ref, recv_ref, send_sem, recv_sem):
        return exchange(
            functools.partial(chip_copy, send_ref, recv_ref, send_sem, recv_sem), chips, chip
        )

    def among_devices(send_ref, recv_ref, send_sem, recv_sem):
        return exchange(
            functools.partial(device_copy, send_ref, recv_ref, send_sem, recv_sem), n, me
        )

    def spread(phase, flat):
        send_ref, recv_ref = token_send.at[phase], token_recv.at[phase]
        for j in range(chips):
            at = j * chip_rows // block * block
            send_ref[j] = flat[:, at : at + block]
        recv_ref[chip] = send_ref[chip]
        return among_chips(
            send_ref, recv_ref, token_send_sem.at[phase], token_recv_sem.at[phase]
        )

    def gathered(phase):
        return jnp.concatenate([token_recv[phase, j] for j in range(chips)], 0).astype(BF16)

    def partial_product(i, segment):
        own_weight[i].wait()
        pull_weight[i].wait_recv()
        product = matmul(segment, weights[i])
        for j in range(chips):
            part_send[i, j] = product[j * rows : (j + 1) * rows].astype(BF16)
        part_recv[i, chip] = part_send[i, chip]
        return among_chips(
            part_send.at[i], part_recv.at[i], part_send_sem.at[i], part_recv_sem.at[i]
        )

    def summed(i):
        total = part_recv[i, 0].astype(F32)
        for j in range(1, chips):
            total = total + part_recv[i, j].astype(F32)
        return total

    copies[0].wait()
    own = tokens[...]
    own_wide = own.astype(F32)
    token_go, token_wait, token_drain = spread(0, own_wide)
    pl.semaphore_wait(barrier, n - 1)
    token_go()
    for copy in push_weight[:3]:
        copy.start()

    for copy in copies[1:15]:
        copy.wait()
    squash = jnp.tanh(matmul_t(own, decay_first[...])).astype(BF16)
    pre_decay = vectors[0] + matmul(squash, decay_second[...])
    softplus = jnp.maximum(-pre_decay, 0.0) + jnp.log(1.0 + jnp.exp(-jnp.abs(pre_decay)))
    decay_rate = jnp.exp(-jnp.exp(-softplus - 0.5))
    low = matmul_t(own, learn_first[...]).astype(BF16)
    learn_rate = sigmoid(vectors[1] + matmul(low, learn_second[...]))
    key_factor = 1.0 + (learn_rate - 1.0) * vectors[2]
    opened = sigmoid(matmul(own, gate_first[...])).astype(BF16)
    gating = matmul(opened, gate_second[...])

    def by_head(i, flat):
        for h in range(head_count):
            heads[i, h * rows : (h + 1) * rows, :] = flat[:, h * head_size : (h + 1) * head_size]

    by_head(0, decay_rate)
    by_head(1, learn_rate)
    by_head(2, key_factor)

    token_wait()
    segment = gathered(0)
    parts = []
    for i in range(3):
        part = partial_product(i, segment)
        part[0]()
        parts.append(part)
    push_weight[3].start()
    parts[0][1]()
    by_head(3, summed(0))
    parts[1][1]()
    value_flat[...] = summed(1)
    parts[2][1]()
    by_head(4, summed(2))

    mask_shape = (head_count, width)
    in_head = (
        lax.broadcasted_iota(jnp.int32, mask_shape, 1) // head_size
        == lax.broadcasted_iota(jnp.int32, mask_shape, 0)
    )
    for t in range(rows):
        decay_t, learn_t, factor_t, key_t, rec_t = [
            heads[i, pl.ds(t, head_count, stride=rows), :] for i in range(5)
        ]
        unit_t = key_t * lax.rsqrt(jnp.sum(key_t * key_t, -1, keepdims=True) + 1e-06)
        written_t = key_t * factor_t
        change_t = unit_t * learn_t
        value_t = jnp.broadcast_to(value_flat[t : t + 1, :], mask_shape)
        probes = jnp.concatenate([unit_t, decay_t * rec_t], 0).astype(BF16)
        state_in[t].wait()
        before = state[t]
        flat_state = before.reshape(width, head_size)
        found = lax.dot_general(
            probes, flat_state.astype(BF16), (((1,), (1,)), ((), ())), preferred_element_type=F32
        )
        removed = found[:head_count]
        change_rec = jnp.sum(change_t * rec_t, -1, keepdims=True)
        written_rec = jnp.sum(written_t * rec_t, -1, keepdims=True)
        own_term = jnp.sum(rec_t * written_t * self_scale[...], -1, keepdims=True)
        readout = jnp.where(
            in_head, found[head_count:] - removed * change_rec + value_t * written_rec, 0.0
        )
        head_mean = jnp.sum(readout, -1, keepdims=True) * (1.0 / head_size)
        head_dev = jnp.where(in_head, readout - head_mean, 0.0)
        head_var = jnp.sum(head_dev * head_dev, -1, keepdims=True) * (1.0 / head_size)
        normed = head_dev * lax.rsqrt(head_var + 0.00064)
        mixed_rows[t : t + 1, :] = jnp.sum(normed, 0, keepdims=True)
        mixed_rows[rows + t : rows + t + 1, :] = jnp.sum(
            jnp.where(in_head, own_term * value_t, 0.0), 0, keepdims=True
        )
        columns[t] = jnp.concatenate(
            [jnp.where(in_head, value_t, 0.0), jnp.where(in_head, -removed, 0.0)], 0
        ).astype(BF16)
        rank_rows[t] = jnp.concatenate([written_t, change_t], 0).astype(BF16)

    normed = mixed_rows[:rows] * vectors[3] + vectors[4]
    mixer_result = ((normed + mixed_rows[rows:]) * gating).astype(BF16).astype(F32)
    mixer_go, mixer_wait, mixer_drain = spread(1, mixer_result)
    mixer_go()
    for t in range(rows):
        decay_t = heads[0, pl.ds(t, head_count, stride=rows), :]
        added = lax.dot_general(
            columns[t], rank_rows[t], (((0,), (0,)), ((), ())), preferred_element_type=F32
        ).reshape(head_count, head_size, head_size)
        for h in range(head_count):
            next_state[t, h] = state[t, h] * decay_t[h : h + 1, :] + added[h]
    mixer_wait()
    out_go, out_wait, out_drain = partial_product(3, gathered(1))
    out_go()

    top = routes.shape[1]
    slots = n * capacity

    def routing(shape, axis):
        slot = lax.broadcasted_iota(jnp.int32, shape, axis)
        expert, place = slot // capacity, lax.rem(slot, capacity)
        earlier = jnp.zeros(shape, jnp.int32)
        held, shares = [], []
        for t in range(rows):
            hit = jnp.zeros(shape, jnp.int32)
            weight = jnp.zeros(shape, F32)
            total = jnp.zeros(shape, F32)
            for k in range(top):
                same = expert == routes[t, k]
                hit = hit + jnp.where(same, 1, 0)
                weight = weight + jnp.where(same, routing_weight[t, k], 0.0)
                total = total + routing_weight[t, k]
            live = (earlier == place) & (hit > 0)
            held.append(jnp.where(live, 1.0, 0.0))
            shares.append(jnp.where(live, weight / total, 0.0))
            earlier = earlier + hit
        return held, shares

    held, _ = routing((slots, 1), 0)
    _, shares = routing((1, slots), 1)
    share_out[...] = jnp.concatenate(shares, 0)

    out_wait()
    hidden = (
        layer_norm(own_wide + summed(3), vectors[5], vectors[6]).astype(BF16).astype(F32)
    )
    hidden_out[...] = hidden
    outgoing = held[0] * hidden[0:1]
    for t in range(1, rows):
        outgoing = outgoing + held[t] * hidden[t : t + 1]
    for e in range(n):
        slot_send[e] = outgoing[e * capacity : (e + 1) * capacity].astype(BF16)
    slot_recv[me] = slot_send[me]
    slot_go, slot_wait, slot_drain = among_devices(
        slot_send, slot_recv, slot_send_sem, slot_recv_sem
    )
    slot_go()
    for copy in copies[15:]:
        copy.wait()
    slot_wait()
    arrived = jnp.concatenate([slot_recv[s].astype(F32) for s in range(n)], 0).astype(BF16)
    gate_val = matmul(arrived, expert_gate[...])
    up_val = matmul(arrived, expert_up[...])
    inner = (gate_val * sigmoid(gate_val) * up_val).astype(BF16)
    produced = matmul(inner, expert_down[...])
    for s in range(n):
        back_send[s] = produced[s * capacity : (s + 1) * capacity].astype(BF16)
    back_recv[me] = back_send[me]
    back_go, back_wait, back_drain = among_devices(
        back_send, back_recv, back_send_sem, back_recv_sem
    )
    back_go()
    token_drain()
    mixer_drain()
    for part in parts:
        part[2]()
    out_drain()
    slot_drain()
    for copy in push_weight:
        copy.wait_send()
    back_wait()
    returned[...] = back_recv[...]
    back_drain()


def finish_kernel(
    state, returned, hidden, share, gain_hbm, bias_hbm, result_hbm, next_hbm, norm, result, sems
):
    rows = state.shape[0]
    copies = [
        pltpu.make_async_copy(gain_hbm, norm.at[0], sems.at[0]),
        pltpu.make_async_copy(bias_hbm, norm.at[1], sems.at[1]),
    ] + [
        pltpu.make_async_copy(state.at[t], next_hbm.at[t], sems.at[2 + t]) for t in range(rows)
    ]
    for copy in copies:
        copy.start()
    share_high = share[...].astype(BF16)
    share_low = (share[...] - share_high.astype(F32)).astype(BF16)
    rows_back = jnp.concatenate(
        [returned[e].astype(F32) for e in range(returned.shape[0])], 0
    ).astype(BF16)
    combined = matmul(share_high, rows_back) + matmul(share_low, rows_back)
    for copy in copies[:2]:
        copy.wait()
    result[...] = layer_norm(hidden[...] + combined, norm[0], norm[1]).astype(BF16)
    last = pltpu.make_async_copy(result, result_hbm, sems.at[2 + rows])
    last.start()
    for copy in copies[2:]:
        copy.wait()
    last.wait()


def body(
    tokens,
    prior_state,
    receptance_matrix,
    key_matrix,
    value_matrix,
    decay_lowrank_first,
    decay_lowrank_second,
    decay_channel_offset,
    correction_lowrank_first,
    correction_lowrank_second,
    correction_offset,
    gate_lowrank_first,
    gate_lowrank_second,
    key_rate_blend,
    self_token_scale,
    per_head_gain,
    per_head_bias,
    mixer_output_weight,
    mixer_norm_gain,
    mixer_norm_bias,
    expert_norm_gain,
    expert_norm_bias,
    routes,
    routing_weight,
    expert_gate_weight,
    expert_up_weight,
    expert_down_weight,
):
    n = lax.axis_size("ep")
    chips = n // 2
    rows, width = tokens.shape
    head_count, head_size = self_token_scale.shape
    capacity = max(2, 2 * rows * routes.shape[1] // n)
    block = max(2 * key_matrix.shape[0], LANES)
    vectors = [
        v.reshape(1, -1)
        for v in (
            decay_channel_offset,
            correction_offset,
            key_rate_blend,
            per_head_gain,
            per_head_bias,
            mixer_norm_gain,
            mixer_norm_bias,
            expert_norm_gain,
            expert_norm_bias,
        )
    ]
    decay_first, learn_first = decay_lowrank_first.T, correction_lowrank_first.T
    anywhere = pl.BlockSpec(memory_space=pltpu.HBM)
    scalars = pl.BlockSpec(memory_space=pltpu.SMEM)
    dma = pltpu.SemaphoreType.DMA
    vmem = pltpu.VMEM
    operands = [
        tokens,
        prior_state,
        key_matrix,
        value_matrix,
        receptance_matrix,
        mixer_output_weight,
        decay_first,
        decay_lowrank_second,
        learn_first,
        correction_lowrank_second,
        gate_lowrank_first,
        gate_lowrank_second,
        *vectors[:7],
        self_token_scale,
        expert_gate_weight,
        expert_up_weight,
        expert_down_weight,
    ]
    passed = pl.pallas_call(
            functools.partial(kernel, n, capacity),
            out_shape=(
                pltpu.VMEM(prior_state.shape, F32),
                pltpu.VMEM((n, capacity, width), BF16),
                pltpu.VMEM(tokens.shape, F32),
                pltpu.VMEM((rows, n * capacity), F32),
            ),
            in_specs=[scalars, scalars] + [anywhere] * len(operands),
            out_specs=(pl.BlockSpec(memory_space=pltpu.VMEM),) * 4,
            scratch_shapes=[
                vmem(tokens.shape, BF16),
                vmem(prior_state.shape, F32),
                vmem((4, block, width), BF16),
                vmem(decay_first.shape, BF16),
                vmem(decay_lowrank_second.shape, BF16),
                vmem(learn_first.shape, BF16),
                vmem(correction_lowrank_second.shape, BF16),
                vmem(gate_lowrank_first.shape, BF16),
                vmem(gate_lowrank_second.shape, BF16),
                vmem((7, 1, width), F32),
                vmem(self_token_scale.shape, F32),
                vmem(expert_gate_weight.shape[1:], BF16),
                vmem(expert_up_weight.shape[1:], BF16),
                vmem(expert_down_weight.shape[1:], BF16),
                vmem((2, chips, rows, block), F32),
                vmem((2, chips, rows, block), F32),
                vmem((4, chips, rows, width), BF16),
                vmem((4, chips, rows, width), BF16),
                vmem((n, capacity, width), BF16),
                vmem((n, capacity, width), BF16),
                vmem((n, capacity, width), BF16),
                vmem((5, head_count * rows, head_size), F32),
                vmem((rows, width), F32),
                vmem((2 * rows, width), F32),
                vmem((rows, 2 * head_count, width), BF16),
                vmem((rows, 2 * head_count, head_size), BF16),
                vmem((n, capacity, width), BF16),
                dma((18,)),
                dma((rows,)),
                dma((4,)),
                dma((4,)),
                dma((4,)),
                dma((2, chips)),
                dma((2, chips)),
                dma((4, chips)),
                dma((4, chips)),
                dma((n,)),
                dma((n,)),
                dma((n,)),
                dma((n,)),
            ],
            compiler_params=pltpu.CompilerParams(
                collective_id=0, has_side_effects=True, vmem_limit_bytes=52 * 1024 * 1024
            ),
        )(routes, routing_weight, *operands)
    inside = pl.BlockSpec(memory_space=pltpu.VMEM)
    return tuple(
        pl.pallas_call(
            finish_kernel,
            out_shape=(
                jax.ShapeDtypeStruct(tokens.shape, BF16),
                jax.ShapeDtypeStruct(prior_state.shape, F32),
            ),
            in_specs=[inside] * 4 + [anywhere] * 2,
            out_specs=(anywhere, anywhere),
            scratch_shapes=[
                vmem((2, 1, width), F32),
                vmem(tokens.shape, BF16),
                dma((rows + 3,)),
            ],
            compiler_params=pltpu.CompilerParams(vmem_limit_bytes=16 * 1024 * 1024),
        )(*passed, *vectors[7:])
    )


def solution(mesh):
    split = P(("grp", "ep"), None)
    state = P(("grp", "ep"), None, None, None)
    matrix = P("ep", None)
    expert = P("ep", None, None)
    in_specs = (
        (split, state)
        + (matrix,) * 3
        + (P(),) * 12
        + (matrix,)
        + (P(),) * 4
        + (split, split)
        + (expert,) * 3
    )
    return jax.shard_map(
        body, mesh=mesh, in_specs=in_specs, out_specs=(split, state), check_vma=False
    )
```
